32 devices in a mesh: grp: 2 (over y), fs: 4 (over z), tp: 4 (over x, core).
Axes of the slice: x: 2, y: 2, z: 4, core: 2. Of those that a mesh axis runs over, the one named last changes fastest.
Arguments:
- tokens: bfloat16 [1024, 2048], P(('grp', 'fs'), 'tp'), parts along dimension 0, may hold values from -40 to 40
- norm_gain: float32 [2048], P('tp'), may hold values from 0.1 to 1.9
- expert_ids: int32 [1024, 8], P(('grp', 'fs')), parts along dimension 0, may hold values from 0 to 63, all different within a row; in each aligned block of 128 rows (0 to 127, 128 to 255, ...) at most 24 rows name the same one
- route_scores: float32 [1024, 8], P(('grp', 'fs')), parts along dimension 0, may hold values from 0.1 to 1
- gate_weight: float32 [64, 512, 2048], P(None, 'fs', 'tp'), may hold values from -0.125 to 0.125
- up_weight: float32 [64, 512, 2048], P(None, 'fs', 'tp'), may hold values from -0.125 to 0.125
- down_weight: float32 [64, 512, 2048], P(None, 'fs', 'tp'), may hold values from -0.25 to 0.25
- shared_gate: float32 [512, 2048], P('fs', 'tp'), may hold values from -0.125 to 0.125
- shared_up: float32 [512, 2048], P('fs', 'tp'), may hold values from -0.125 to 0.125
- shared_down: float32 [512, 2048], P('fs', 'tp'), may hold values from -0.25 to 0.25
Outputs:
- gate_served: bfloat16 [128, 512, 2048], P(('grp', 'fs'), None, 'tp'), parts along dimension 0
- up_served: bfloat16 [128, 512, 2048], P(('grp', 'fs'), None, 'tp'), parts along dimension 0
- down_served: bfloat16 [128, 512, 2048], P(('grp', 'fs'), None, 'tp'), parts along dimension 0
- shared_gate_served: bfloat16 [1024, 2048], P('grp', 'tp'), parts along dimension 0
- shared_up_served: bfloat16 [1024, 2048], P('grp', 'tp'), parts along dimension 0
- shared_down_served: bfloat16 [1024, 2048], P('grp', 'tp'), parts along dimension 0
- layer_output: bfloat16 [1024, 2048], P(('grp', 'fs'), 'tp'), parts along dimension 0
The draws below stay inside these ranges and needn't reach their ends.
There are 2 independent parts, one for each index of `grp`. The reference program is written for one: setup_inputs(seed, part) draws one part's arguments, and reference() takes and returns one part's arrays. A program takes and returns all parts, laid end to end along the dimension named above; an argument that names none is the same for every part. Nothing has to cross between parts.
Inputs may be any that keep to these rules, and one draw needn't show every extreme that they name: `expert_ids`: each row names 8 different experts. Among the rows of one index of fs no expert is named more than 24 times; in every draw some expert reaches 24 on some index of fs.
All inputs are finite; a program needn't handle non-finite values.
Results may differ from the reference program's by a relative error of at most 0.03.
Values may be sent and summed in bfloat16 or wider, within the bound.
A program may use at most 192 MiB of HBM per device.

```python
import math
import jax
import jax.numpy as jnp
import numpy as np
from jax import lax

D = 2048
FF = 512
EXPERTS = 64
TOP_K = 8
TOK_DEV = 128
CAPACITY = 24
TOKENS = 512
N_FS = 4
N_TP = 4


def draw_tokens(key, part):
    draw_key = jax.random.fold_in(key, 0)
    column = 3.0 ** (jnp.arange(D, dtype=jnp.float32) / (D - 1))
    values = jnp.clip(jax.random.normal(draw_key, (TOKENS, D), jnp.float32), -8.0, 8.0)
    return (values * column[None, :]).astype(jnp.bfloat16)


def levels(rng, extent, cuts, smallest, top_value):
    def one(dim, shards_of):
        heights = jax.random.uniform(jax.random.fold_in(jax.random.fold_in(rng, 6), dim), (shards_of,), jnp.float32, smallest / len(cuts), top_value / len(cuts))
        return jnp.repeat(jnp.exp(heights), extent[dim] // shards_of).reshape((-1,) + (1,) * (len(extent) - dim - 1))

    loudness = one(*cuts[0])
    for cut in cuts[1:]:
        loudness = loudness * one(*cut)
    return loudness


def assign_block(stream_key, own, number, rows, number_of, top, most, lean):
    sequence = jax.random.permutation(stream_key, number_of)
    heavy_load, common = load_shares(number_of, rows * top, most, lean, True), load_shares(number_of, rows * top, most, lean, False)
    places = jnp.arange(number_of)

    def named(lengths, rotation):
        used = int((lengths > 0).sum())
        fixed = max(1, used // 4)
        passed = fixed + (places - fixed + rotation * (used - fixed)) % max(1, number_of - fixed)
        return jnp.zeros((number_of,), jnp.int32).at[sequence[jnp.where(places < fixed, places, passed)]].set(jnp.asarray(lengths, jnp.int32))

    lengths = jnp.where(number % 4 == 0, named(heavy_load, number // 4), named(common, number - number // 4 - 1))
    mixed = jax.random.permutation(jax.random.fold_in(own, 3), number_of)
    source_of, receiver = mixed[0:number_of // 2 * 2:2], mixed[1:number_of // 2 * 2:2]
    margin = jnp.minimum(lengths[source_of] - 1, most - lengths[receiver]) // 2
    margin = jnp.where((source_of == sequence[0]) | (receiver == sequence[0]) | (lengths[receiver] == 0), 0, jnp.maximum(margin, 0))
    passed = jax.random.randint(jax.random.fold_in(own, 4), (number_of // 2,), 0, 1 << 20) % (margin + 1)
    lengths = lengths.at[source_of].add(-passed).at[receiver].add(passed)
    members = jnp.searchsorted(jnp.cumsum(lengths), jnp.arange(rows * top), side="right").astype(jnp.int32)
    table = members.reshape(top, rows).T
    table = table[jax.random.permutation(jax.random.fold_in(own, 1), rows)]
    rotation = jax.random.randint(jax.random.fold_in(own, 2), (rows, 1), 0, top)
    return jnp.take_along_axis(table, (jnp.arange(top)[None, :] + rotation) % top, axis=1)


def load_shares(amount, total, most, lean, full):
    loads = [(1 << 20) // math.isqrt(standing ** lean) + 1 for standing in range(1, amount + 1)]
    largest = most if full else min(most, max(-(-total // amount), total * loads[0] // sum(loads)))
    least = 1 if total - largest >= amount - 1 else 0
    counts, spare = [largest] + [least] * (amount - 1), total - largest - least * (amount - 1)
    while spare > 0:
        movable = [i for i in range(1, amount) if counts[i] < largest] or [i for i in range(1, amount) if counts[i] < most]
        mass, remaining = sum([loads[i] for i in movable]), spare
        for i in movable:
            addition = min(most - counts[i], max(1, remaining * loads[i] // mass), spare)
            counts[i] = counts[i] + addition
            spare = spare - addition
    return np.array(counts)


def centred(key, shape, deviation, limit, cuts=(), kind=jnp.bfloat16):
    level = levels(key, shape, cuts, -0.22, 0.18) if cuts else 1.0
    array = jax.random.normal(key, shape, jnp.float32) * deviation * level
    return jnp.minimum(jnp.maximum(array, -limit), limit).astype(kind)


def setup_inputs(seed: int = 0, part: int = 0) -> dict:
    key_of = jax.random.split(jax.random.key(seed), 11)
    own_keys = jax.random.split(jax.random.fold_in(key_of[10], part), 11)
    tokens = draw_tokens(jax.random.fold_in(jax.random.fold_in(key_of[10], part), 71), part)
    norm_gain = jnp.clip(1.0 + 0.18 * jax.random.normal(key_of[1], (D,), jnp.float32), 0.1, 1.9)
    expert_ids_keys = jax.random.split(jax.random.fold_in(own_keys[2], 1), TOKENS // TOK_DEV)
    expert_ids_turns = jax.random.permutation(jax.random.fold_in(own_keys[2], 3), TOKENS // TOK_DEV)
    expert_ids = jax.vmap(lambda own, number: assign_block(jax.random.fold_in(own_keys[2], 2), own, number, TOK_DEV, EXPERTS, TOP_K, CAPACITY, 2))(expert_ids_keys, expert_ids_turns).reshape((TOKENS, TOP_K))
    route_scores = jnp.clip(jnp.exp(math.log(1.0) - 2.3025851 * jax.random.uniform(own_keys[3], (TOKENS, TOP_K), jnp.float32) ** levels(own_keys[3], (TOKENS, TOP_K), ((0, 4),), -0.2, 0.2)), 0.1, 1.0)
    gate_weight = centred(key_of[4], (EXPERTS, FF, D), D ** -0.5, 0.125, ((1, 4), (2, 4)), jnp.float32)
    up_weight = centred(key_of[5], (EXPERTS, FF, D), D ** -0.5, 0.125, ((1, 4), (2, 4)), jnp.float32)
    down_weight = centred(key_of[6], (EXPERTS, FF, D), FF ** -0.5, 0.25, ((1, 4), (2, 4)), jnp.float32)
    shared_gate = centred(key_of[7], (FF, D), D ** -0.5, 0.125, ((0, 4), (1, 4)), jnp.float32)
    shared_up = centred(key_of[8], (FF, D), D ** -0.5, 0.125, ((0, 4), (1, 4)), jnp.float32)
    shared_down = centred(key_of[9], (FF, D), FF ** -0.5, 0.25, ((0, 4), (1, 4)), jnp.float32)
    return dict(tokens=tokens, norm_gain=norm_gain, expert_ids=expert_ids, route_scores=route_scores, gate_weight=gate_weight, up_weight=up_weight, down_weight=down_weight, shared_gate=shared_gate, shared_up=shared_up, shared_down=shared_down)


norm_eps = 1e-05
routed_scale = 2.5

def normalize(tokens):
    tok_float = tokens.astype(jnp.float32)
    full_width = tok_float.shape[1]
    row_mean = lax.optimization_barrier(jnp.sum(tok_float, axis=1)) / full_width
    row_var = lax.optimization_barrier(jnp.sum(tok_float * tok_float, axis=1)) / full_width - row_mean * row_mean
    return ((tok_float - row_mean[:, None]) * lax.rsqrt(row_var + norm_eps)[:, None]).astype(jnp.bfloat16)

def blocked_hidden(rows_in, paired):
    count_rows = rows_in.shape[0]
    split_rows = rows_in.astype(jnp.float32).reshape(count_rows, N_TP, -1)
    split_pair = paired.astype(jnp.float32).reshape(paired.shape[0], N_TP, -1)
    partial_value = jnp.einsum('ntd,ftd->tnf', split_rows, split_pair).astype(jnp.bfloat16)
    summed = lax.optimization_barrier(jnp.sum(partial_value.astype(jnp.float32), axis=0))
    return (jax.nn.silu(summed[:, :FF]) * summed[:, FF:]).astype(jnp.bfloat16)

def reference(tokens, norm_gain, expert_ids, route_scores, gate_weight, up_weight, down_weight, shared_gate, shared_up, shared_down):
    normed = normalize(tokens)
    gate_new = (gate_weight * norm_gain[None, None, :]).astype(jnp.bfloat16)
    up_new = (up_weight * norm_gain[None, None, :]).astype(jnp.bfloat16)
    down_new = down_weight.astype(jnp.bfloat16)
    gate_shared = (shared_gate * norm_gain[None, :]).astype(jnp.bfloat16)
    up_shared = (shared_up * norm_gain[None, :]).astype(jnp.bfloat16)
    down_shared = shared_down.astype(jnp.bfloat16)
    route_weight = route_scores / lax.optimization_barrier(jnp.sum(route_scores, axis=1, keepdims=True)) * routed_scale
    flat_ids = expert_ids.reshape(-1)
    assignments = flat_ids.shape[0]
    flat_tokens = jnp.concatenate([jnp.arange(assignments, dtype=jnp.int32) // TOP_K, jnp.full((1,), TOKENS, jnp.int32)])
    flat_weight = jnp.concatenate([route_weight.reshape(-1), jnp.zeros((1,), jnp.float32)])
    padded = jnp.concatenate([normed, jnp.zeros((1, D), jnp.bfloat16)], axis=0)

    def one_expert(running, expert):
        chosen = jnp.nonzero(flat_ids == expert, size=N_FS * CAPACITY, fill_value=assignments)[0].astype(jnp.int32)
        token_rows = flat_tokens[chosen]
        paired = jnp.concatenate([gate_new[expert], up_new[expert]], axis=0)
        hidden = blocked_hidden(padded[token_rows], paired)
        result = jnp.dot(hidden, down_new[expert], preferred_element_type=jnp.float32).astype(jnp.bfloat16)
        return (running.at[token_rows].add(result.astype(jnp.float32) * flat_weight[chosen][:, None]), None)
    routed, _ = lax.scan(one_expert, jnp.zeros((TOKENS + 1, D), jnp.float32), jnp.arange(EXPERTS, dtype=jnp.int32))
    shared_hidden = blocked_hidden(normed, jnp.concatenate([gate_shared, up_shared], axis=0))
    shared_out = jnp.dot(shared_hidden, down_shared, preferred_element_type=jnp.float32)
    layer_out = (shared_out + routed[:TOKENS]).astype(jnp.bfloat16)
    return (gate_new, up_new, down_new, gate_shared, up_shared, down_shared, layer_out)
```

```python
import jax
import jax.numpy as jnp
from jax import lax
from jax.sharding import PartitionSpec as P

CAPACITY = 24


norm_eps = 1e-05
routed_scale = 2.5
DEPTH = 2
SUBS = 2


def partner_lists(count):
    power = count & (count - 1) == 0
    return [[(i ^ k) if power else (i + k) % count for i in range(count)] for k in range(1, count)]


def exchange(weights, gain, served):
    shard_count = lax.axis_size("fs")
    groups = lax.axis_size("grp")
    me = lax.axis_index("fs")
    grp = lax.axis_index("grp")
    experts_all, hidden_part, width = weights[0].shape
    here = experts_all // shard_count
    two = groups == 2 and here % 2 == 0

    def block(m, first, count):
        piece = lax.dynamic_slice_in_dim(weights[m], first, count, 0)
        if gain[m] is not None:
            piece = piece * gain[m][None, None, :]
        return piece.astype(jnp.bfloat16)

    outs = []
    for m in range(len(weights)):
        own = lax.dynamic_slice_in_dim(served[m], me * here, here, 0)
        base = jnp.zeros((here, hidden_part * shard_count, width), jnp.bfloat16)
        outs.append(lax.dynamic_update_slice(base, own, (0, me * hidden_part, 0)))

    lanes = []
    for k, partners in enumerate(partner_lists(shard_count), start=1):
        to = jnp.asarray(partners, jnp.int32)[me]
        source = [0] * shard_count
        for i, j in enumerate(partners):
            source[j] = i
        origin = jnp.asarray(source, jnp.int32)[me]
        lanes.append((k, partners, to, origin, two and k > 1))
    lanes = lanes[1:] + lanes[:1]
    history = {lane[0]: [] for lane in lanes}
    for m in range(len(weights)):
        span = {True: here // 2, False: here}
        for part in range(SUBS if (here // 2) % SUBS == 0 else 1):
            parts = SUBS if (here // 2) % SUBS == 0 else 1
            for k, partners, to, origin, split in lanes:
                count = span[split] // parts
                offset = part * count
                if split:
                    offset = offset + grp * (here // 2)
                piece = block(m, to * here + offset, count)
                past = history[k]
                if len(past) >= DEPTH:
                    piece, past[-DEPTH] = lax.optimization_barrier((piece, past[-DEPTH]))
                got = lax.ppermute(piece, "fs", list(enumerate(partners)))
                past.append(got)
                outs[m] = lax.dynamic_update_slice(outs[m], got, (offset, origin * hidden_part, 0))
                if split:
                    other = lax.ppermute(got, "grp", [(0, 1), (1, 0)])
                    offset = part * count + (1 - grp) * (here // 2)
                    outs[m] = lax.dynamic_update_slice(
                        outs[m], other, (offset, origin * hidden_part, 0)
                    )
    return outs


def on_device(
    tokens,
    norm_gain,
    expert_ids,
    route_scores,
    gate_weight,
    up_weight,
    down_weight,
    shared_gate,
    shared_up,
    shared_down,
):
    shard_count = lax.axis_size("fs")
    me = lax.axis_index("fs")
    experts_all = gate_weight.shape[0]
    tok_rows, top_count = expert_ids.shape
    slots = shard_count * CAPACITY

    tok_float = tokens.astype(jnp.float32)
    row_sum, row_squares = lax.psum(
        (jnp.sum(tok_float, axis=1), jnp.sum(tok_float * tok_float, axis=1)), "tp"
    )
    full_width = tok_float.shape[1] * lax.axis_size("tp")
    row_mean = row_sum / full_width
    row_var = row_squares / full_width - row_mean * row_mean
    normed = ((tok_float - row_mean[:, None]) * lax.rsqrt(row_var + norm_eps)[:, None]).astype(
        jnp.bfloat16
    )

    route_weight = route_scores / jnp.sum(route_scores, axis=1, keepdims=True) * routed_scale
    chosen = expert_ids[:, :, None] == jnp.arange(experts_all, dtype=jnp.int32)[None, None, :]
    named = jnp.any(chosen, axis=1)
    dense_weight = jnp.sum(jnp.where(chosen, route_weight[:, :, None], 0.0), axis=1)
    below = (
        jnp.arange(tok_rows)[:, None] > jnp.arange(tok_rows)[None, :]
    ).astype(jnp.bfloat16)
    rank = jnp.dot(below, named.astype(jnp.bfloat16), preferred_element_type=jnp.float32)
    slot = jnp.where(named, rank + (me * CAPACITY).astype(jnp.float32), -1.0)
    routing = lax.all_gather(
        jnp.concatenate([slot, dense_weight], axis=1), "fs", axis=0, tiled=True
    )
    tokens_here = lax.all_gather(normed, "fs", axis=0, tiled=True)

    gate_new = (gate_weight * norm_gain[None, None, :]).astype(jnp.bfloat16)
    up_new = (up_weight * norm_gain[None, None, :]).astype(jnp.bfloat16)
    down_new = down_weight.astype(jnp.bfloat16)
    gate_shared = (shared_gate * norm_gain[None, :]).astype(jnp.bfloat16)
    up_shared = (shared_up * norm_gain[None, :]).astype(jnp.bfloat16)
    down_shared = shared_down.astype(jnp.bfloat16)
    gate_whole, up_whole, down_whole = (
        lax.all_gather(gate_shared, "fs", axis=0, tiled=True),
        lax.all_gather(up_shared, "fs", axis=0, tiled=True),
        lax.all_gather(down_shared, "fs", axis=0, tiled=True),
    )
    gate_local, up_local, down_local = exchange(
        (gate_weight, up_weight, down_weight),
        (norm_gain, norm_gain, None),
        (gate_new, up_new, down_new),
    )

    slot_of = routing[:, :experts_all].T
    weight_of = routing[:, experts_all:].T
    select = slot_of[:, None, :] == jnp.arange(slots, dtype=jnp.float32)[None, :, None]
    pick = select.astype(jnp.bfloat16)
    slot_weight = jnp.sum(jnp.where(select, weight_of[:, None, :], 0.0), axis=2)
    rows = jnp.einsum(
        "est,td->esd", pick, tokens_here, preferred_element_type=jnp.float32
    ).astype(jnp.bfloat16)
    hidden_width = gate_weight.shape[1]
    routed_rows = experts_all * slots

    def terms(routed, shared):
        out = jnp.einsum("esd,efd->esf", rows, routed, preferred_element_type=jnp.float32)
        own = lax.dot_general(
            tokens_here, shared, (((1,), (1,)), ((), ())), preferred_element_type=jnp.float32
        )
        return jnp.concatenate(
            [out.astype(jnp.bfloat16).reshape(routed_rows, hidden_width), own.astype(jnp.bfloat16)],
            axis=0,
        )

    all_terms = jnp.concatenate([terms(gate_new, gate_shared), terms(up_new, up_shared)], axis=1)
    row_share = lax.psum_scatter(all_terms, "tp", scatter_dimension=0, tiled=True).astype(
        jnp.float32
    )
    hidden_part = (jax.nn.silu(row_share[:, :hidden_width]) * row_share[:, hidden_width:]).astype(
        jnp.bfloat16
    )
    hidden = lax.all_gather(hidden_part, "tp", axis=0, tiled=True)
    expert_hidden = hidden[:routed_rows].reshape(experts_all, slots, hidden_width)
    results = jnp.einsum(
        "esf,efd->esd", expert_hidden, down_new, preferred_element_type=jnp.float32
    )
    weighted = (results * slot_weight[:, :, None]).astype(jnp.bfloat16)
    routed = jnp.einsum("est,esd->td", pick, weighted, preferred_element_type=jnp.float32)
    shared_out = jnp.dot(hidden[routed_rows:], down_shared, preferred_element_type=jnp.float32)
    layer_out = lax.psum_scatter(
        (shared_out + routed).astype(jnp.bfloat16), "fs", scatter_dimension=0, tiled=True
    )
    return (gate_local, up_local, down_local, gate_whole, up_whole, down_whole, layer_out)


def solution(mesh):
    in_specs = (
        P(("grp", "fs"), "tp"),
        P("tp"),
        P(("grp", "fs"), None),
        P(("grp", "fs"), None),
        P(None, "fs", "tp"),
        P(None, "fs", "tp"),
        P(None, "fs", "tp"),
        P("fs", "tp"),
        P("fs", "tp"),
        P("fs", "tp"),
    )
    out_specs = (
        P(("grp", "fs"), None, "tp"),
        P(("grp", "fs"), None, "tp"),
        P(("grp", "fs"), None, "tp"),
        P("grp", "tp"),
        P("grp", "tp"),
        P("grp", "tp"),
        P(("grp", "fs"), "tp"),
    )
    return jax.shard_map(
        on_device, mesh=mesh, in_specs=in_specs, out_specs=out_specs, check_vma=False
    )
```

```python
import jax
import jax.numpy as jnp
from jax import lax
from jax.sharding import PartitionSpec as P

CAPACITY = 24


norm_eps = 1e-05
routed_scale = 2.5
DEPTH = 3
SUBS = 2


def partner_lists(count):
    power = count & (count - 1) == 0
    return [[(i ^ k) if power else (i + k) % count for i in range(count)] for k in range(1, count)]


def exchange(weights, gain, served, after):
    shard_count = lax.axis_size("fs")
    groups = lax.axis_size("grp")
    me = lax.axis_index("fs")
    grp = lax.axis_index("grp")
    experts_all, hidden_part, width = weights[0].shape
    here = experts_all // shard_count
    two = groups == 2 and here % 2 == 0

    def block(m, first, count):
        piece = lax.dynamic_slice_in_dim(weights[m], first, count, 0)
        if gain[m] is not None:
            piece = piece * gain[m][None, None, :]
        return piece.astype(jnp.bfloat16)

    outs = []
    for m in range(len(weights)):
        own = lax.dynamic_slice_in_dim(served[m], me * here, here, 0)
        base = jnp.zeros((here, hidden_part * shard_count, width), jnp.bfloat16)
        outs.append(lax.dynamic_update_slice(base, own, (0, me * hidden_part, 0)))

    lanes = []
    for k, partners in enumerate(partner_lists(shard_count), start=1):
        to = jnp.asarray(partners, jnp.int32)[me]
        source = [0] * shard_count
        for i, j in enumerate(partners):
            source[j] = i
        origin = jnp.asarray(source, jnp.int32)[me]
        lanes.append((k, partners, to, origin, two and k > 1))
    lanes = lanes[1:] + lanes[:1]
    history = {lane[0]: [] for lane in lanes}
    parts = SUBS if (here // 2) % SUBS == 0 else 1
    span = {True: here // 2, False: here}

    def piece_of(m, part, to, split):
        count = span[split] // parts
        offset = part * count
        if split:
            offset = offset + grp * (here // 2)
        return block(m, to * here + offset, count), count, offset

    opening = [piece_of(0, 0, to, split)[0] for _, _, to, _, split in lanes]
    after, *opening = lax.optimization_barrier((after, *opening))
    opened = []
    for m in range(len(weights)):
        for part in range(parts):
            for lane, (k, partners, to, origin, split) in enumerate(lanes):
                piece, count, offset = piece_of(m, part, to, split)
                if m == 0 and part == 0:
                    piece = opening[lane]
                past = history[k]
                if len(past) >= DEPTH:
                    piece, past[-DEPTH] = lax.optimization_barrier((piece, past[-DEPTH]))
                got = lax.ppermute(piece, "fs", list(enumerate(partners)))
                if m == 0 and part == 0:
                    opened.append(got)
                    if len(opened) == len(lanes):
                        after, *opened = lax.optimization_barrier((after, *opened))
                past.append(got)
                outs[m] = lax.dynamic_update_slice(outs[m], got, (offset, origin * hidden_part, 0))
                if split:
                    other = lax.ppermute(got, "grp", [(0, 1), (1, 0)])
                    offset = part * count + (1 - grp) * (here // 2)
                    outs[m] = lax.dynamic_update_slice(
                        outs[m], other, (offset, origin * hidden_part, 0)
                    )
    return outs, after


def on_device(
    tokens,
    norm_gain,
    expert_ids,
    route_scores,
    gate_weight,
    up_weight,
    down_weight,
    shared_gate,
    shared_up,
    shared_down,
):
    shard_count = lax.axis_size("fs")
    me = lax.axis_index("fs")
    experts_all = gate_weight.shape[0]
    tok_rows, top_count = expert_ids.shape
    slots = shard_count * CAPACITY

    tok_float = tokens.astype(jnp.float32)
    row_sum, row_squares = lax.psum(
        (jnp.sum(tok_float, axis=1), jnp.sum(tok_float * tok_float, axis=1)), "tp"
    )
    full_width = tok_float.shape[1] * lax.axis_size("tp")
    row_mean = row_sum / full_width
    row_var = row_squares / full_width - row_mean * row_mean
    normed = ((tok_float - row_mean[:, None]) * lax.rsqrt(row_var + norm_eps)[:, None]).astype(
        jnp.bfloat16
    )

    route_weight = route_scores / jnp.sum(route_scores, axis=1, keepdims=True) * routed_scale
    chosen = expert_ids[:, :, None] == jnp.arange(experts_all, dtype=jnp.int32)[None, None, :]
    named = jnp.any(chosen, axis=1)
    dense_weight = jnp.sum(jnp.where(chosen, route_weight[:, :, None], 0.0), axis=1)
    below = (
        jnp.arange(tok_rows)[:, None] > jnp.arange(tok_rows)[None, :]
    ).astype(jnp.bfloat16)
    rank = jnp.dot(below, named.astype(jnp.bfloat16), preferred_element_type=jnp.float32)
    slot = jnp.where(named, rank + (me * CAPACITY).astype(jnp.float32), -1.0)
    gate_new = (gate_weight * norm_gain[None, None, :]).astype(jnp.bfloat16)
    up_new = (up_weight * norm_gain[None, None, :]).astype(jnp.bfloat16)
    down_new = down_weight.astype(jnp.bfloat16)
    gate_shared = (shared_gate * norm_gain[None, :]).astype(jnp.bfloat16)
    up_shared = (shared_up * norm_gain[None, :]).astype(jnp.bfloat16)
    down_shared = shared_down.astype(jnp.bfloat16)
    high = lax.reduce_precision(dense_weight, 8, 7)
    middle = lax.reduce_precision(dense_weight - high, 8, 7)
    low = dense_weight - high - middle
    routing = jnp.concatenate([slot, high, middle, low], axis=1).astype(jnp.bfloat16)
    width = normed.shape[1]
    columns = routing.shape[1]
    lines = -(-columns // width)
    routing = jnp.pad(routing, ((0, 0), (0, lines * width - columns)))
    small = jnp.concatenate(
        [gate_shared, up_shared, down_shared, normed]
        + [routing[:, i * width : (i + 1) * width] for i in range(lines)],
        axis=0,
    )
    gathered = lax.all_gather(small, "fs", axis=0, tiled=False)
    (gate_local, up_local, down_local), gathered_late = exchange(
        (gate_weight, up_weight, down_weight),
        (norm_gain, norm_gain, None),
        (gate_new, up_new, down_new),
        gathered,
    )
    shared_part = shared_gate.shape[0]
    gate_whole, up_whole, down_whole = (
        gathered_late[:, i * shared_part : (i + 1) * shared_part].reshape(-1, width)
        for i in range(3)
    )
    start = 3 * shared_part
    tokens_here = gathered_late[:, start : start + tok_rows].reshape(-1, width)
    start = start + tok_rows
    routing = jnp.concatenate(
        [
            gathered_late[:, start + i * tok_rows : start + (i + 1) * tok_rows].reshape(-1, width)
            for i in range(lines)
        ],
        axis=1,
    )[:, :columns].astype(jnp.float32)
    slot_all, high, middle, low = (
        routing[:, i * experts_all : (i + 1) * experts_all] for i in range(4)
    )

    slot_of = slot_all.T
    weight_of = (high + middle + low).T
    select = slot_of[:, None, :] == jnp.arange(slots, dtype=jnp.float32)[None, :, None]
    pick = select.astype(jnp.bfloat16)
    slot_weight = jnp.sum(jnp.where(select, weight_of[:, None, :], 0.0), axis=2)
    rows = jnp.einsum(
        "est,td->esd", pick, tokens_here, preferred_element_type=jnp.float32
    ).astype(jnp.bfloat16)
    hidden_width = gate_weight.shape[1]
    routed_rows = experts_all * slots

    def terms(routed, shared):
        out = jnp.einsum("esd,efd->esf", rows, routed, preferred_element_type=jnp.float32)
        own = lax.dot_general(
            tokens_here, shared, (((1,), (1,)), ((), ())), preferred_element_type=jnp.float32
        )
        return jnp.concatenate(
            [out.astype(jnp.bfloat16).reshape(routed_rows, hidden_width), own.astype(jnp.bfloat16)],
            axis=0,
        )

    all_terms = jnp.concatenate([terms(gate_new, gate_shared), terms(up_new, up_shared)], axis=1)
    row_share = lax.psum_scatter(all_terms, "tp", scatter_dimension=0, tiled=True).astype(
        jnp.float32
    )
    hidden_part = (jax.nn.silu(row_share[:, :hidden_width]) * row_share[:, hidden_width:]).astype(
        jnp.bfloat16
    )
    hidden = lax.all_gather(hidden_part, "tp", axis=0, tiled=True)
    expert_hidden = hidden[:routed_rows].reshape(experts_all, slots, hidden_width)
    results = jnp.einsum(
        "esf,efd->esd", expert_hidden, down_new, preferred_element_type=jnp.float32
    )
    weighted = (results * slot_weight[:, :, None]).astype(jnp.bfloat16)
    routed = jnp.einsum("est,esd->td", pick, weighted, preferred_element_type=jnp.float32)
    shared_out = jnp.dot(hidden[routed_rows:], down_shared, preferred_element_type=jnp.float32)
    layer_out = lax.psum_scatter(
        (shared_out + routed).astype(jnp.bfloat16), "fs", scatter_dimension=0, tiled=True
    )
    return (gate_local, up_local, down_local, gate_whole, up_whole, down_whole, layer_out)


def solution(mesh):
    in_specs = (
        P(("grp", "fs"), "tp"),
        P("tp"),
        P(("grp", "fs"), None),
        P(("grp", "fs"), None),
        P(None, "fs", "tp"),
        P(None, "fs", "tp"),
        P(None, "fs", "tp"),
        P("fs", "tp"),
        P("fs", "tp"),
        P("fs", "tp"),
    )
    out_specs = (
        P(("grp", "fs"), None, "tp"),
        P(("grp", "fs"), None, "tp"),
        P(("grp", "fs"), None, "tp"),
        P("grp", "tp"),
        P("grp", "tp"),
        P("grp", "tp"),
        P(("grp", "fs"), "tp"),
    )
    return jax.shard_map(
        on_device, mesh=mesh, in_specs=in_specs, out_specs=out_specs, check_vma=False
    )
```
